32 devices in a mesh: ep: 8 (over z, y), tp: 4 (over x, core).
Axes of the slice: x: 2, y: 2, z: 4, core: 2. Of those that a mesh axis runs over, the one named last changes fastest.
Arguments:
- queries: bfloat16 [4096, 2048], P('ep', 'tp'), may hold values from -6 to 6
- forget_pre: float32 [4096, 2048], P('ep', 'tp'), may hold values from -8 to 20
- value_in: bfloat16 [4096, 2048], P('ep', 'tp'), may hold values from -6 to 6
- out_gate: bfloat16 [4096, 2048], P('ep', 'tp'), may hold values from -6 to 6
- lower_bound: float32 [2048], P('tp'), may hold values from 0.5 to 0.8
- out_gain: float32 [128], replicated, may hold values from 0.1 to 1.9
- out_weight: bfloat16 [2048, 2048], P('tp'), may hold values from -0.125 to 0.125
- moe_tokens: bfloat16 [2048, 2048], P('ep'), may hold values from -6 to 6
- moe_gain: float32 [2048], replicated, may hold values from 0.1 to 1.9
- expert_ids: int32 [2048, 4], P('ep'), may hold values from 0 to 15, all different within a row; in each aligned block of 64 rows (0 to 63, 64 to 127, ...) at most 32 rows name the same one
- route_weights: float32 [2048, 4], P('ep'), may hold values from 0.1 to 1
- w_gate: bfloat16 [16, 2048, 1024], P('ep', None, 'tp'), may hold values from -0.125 to 0.125
- w_up: bfloat16 [16, 2048, 1024], P('ep', None, 'tp'), may hold values from -0.125 to 0.125
- w_down: bfloat16 [16, 1024, 2048], P('ep', 'tp'), may hold values from -0.1875 to 0.1875
Outputs:
- mixer_out: bfloat16 [4096, 2048], P(('ep', 'tp'))
- expert_out: bfloat16 [2048, 2048], P(('ep', 'tp'))
The draws below stay inside these ranges and needn't reach their ends.
Inputs may be any that keep to these rules, and one draw needn't show every extreme that they name: `expert_ids`: each row names 4 different experts. In each aligned block of 64 rows no expert is named by more than 32 rows, and in some block some expert is named by exactly 32 rows.
All inputs are finite; a program needn't handle non-finite values.
Results may differ from the reference program's by a relative error of at most 0.01065.
Values may be sent and summed in bfloat16 or wider, within the bound.
A program may use at most 128 MiB of HBM per device.

```python
import math
import jax
import jax.numpy as jnp
import numpy as np
from jax import lax

D = 2048
HEAD_DIM = 128
BLOCK = 64
FE = 1024
EXPERTS = 16
TOPK = 4
SEQ_DEV = 512
SEQUENCE_TOTAL = 4096
MOE_ALL = 2048
QROWS = 64
CAPQ = 32
N_TP = 4


def draw_forget_pre(key, part):
    random_subkeys = jax.random.split(key, 6)
    slow_share = 0.6
    slow_mask = jax.random.uniform(random_subkeys[0], (D,)) < slow_share
    reach_factor = jax.random.uniform(random_subkeys[1], (D,), minval=0.5, maxval=2.0)
    fast_rate = 1.0 / jax.random.uniform(random_subkeys[2], (D,), minval=30.0, maxval=60.0)
    target = jnp.where(slow_mask, reach_factor / SEQUENCE_TOTAL, fast_rate)
    level_floor = jnp.log(0.35 / target)
    block_shift = jax.random.uniform(random_subkeys[3], (SEQUENCE_TOTAL // SEQ_DEV, 1), minval=-0.7, maxval=0.7)
    level_per_block = jnp.repeat(block_shift, SEQ_DEV, axis=0)
    random_noise = 0.7 * jax.random.truncated_normal(random_subkeys[4], -5.0, 5.0, (SEQUENCE_TOTAL, D))
    spike_events = jax.random.randint(random_subkeys[5], (6,), 0, SEQUENCE_TOTAL)
    position_indices = jnp.arange(SEQUENCE_TOTAL)
    spike_mask = jnp.any(position_indices[:, None] == spike_events[None, :], axis=1)
    sampled_values = jnp.where(spike_mask[:, None], -4.0 + 0.3 * random_noise, level_floor[None, :] + level_per_block + random_noise)
    return sampled_values.astype(jnp.float32)


def shard_levels(rng, extent, cuts, smallest, largest):
    def one(axis_at, parts):
        heights = jax.random.uniform(jax.random.fold_in(jax.random.fold_in(rng, 6), axis_at), (parts,), jnp.float32, smallest / len(cuts), largest / len(cuts))
        return jnp.repeat(jnp.exp(heights), extent[axis_at] // parts).reshape((-1,) + (1,) * (len(extent) - axis_at - 1))

    loudness = one(*cuts[0])
    for cut in cuts[1:]:
        loudness = loudness * one(*cut)
    return loudness


def deal_out(key, own, number, rows, count, top, bound, slope):
    ranking = jax.random.permutation(key, count)
    crowded, ordinary = shares(count, rows * top, bound, slope, True), shares(count, rows * top, bound, slope, False)
    places = jnp.arange(count)

    def named(tallies, turn):
        used = int((tallies > 0).sum())
        fixed = max(1, used // 4)
        shifted = fixed + (places - fixed + turn * (used - fixed)) % max(1, count - fixed)
        return jnp.zeros((count,), jnp.int32).at[ranking[jnp.where(places < fixed, places, shifted)]].set(jnp.asarray(tallies, jnp.int32))

    tallies = jnp.where(number % 4 == 0, named(crowded, number // 4), named(ordinary, number - number // 4 - 1))
    mixed = jax.random.permutation(jax.random.fold_in(own, 3), count)
    donor, receiver = mixed[0:count // 2 * 2:2], mixed[1:count // 2 * 2:2]
    room = jnp.minimum(tallies[donor] - 1, bound - tallies[receiver]) // 2
    room = jnp.where((donor == ranking[0]) | (receiver == ranking[0]) | (tallies[receiver] == 0), 0, jnp.maximum(room, 0))
    shifted = jax.random.randint(jax.random.fold_in(own, 4), (count // 2,), 0, 1 << 20) % (room + 1)
    tallies = tallies.at[donor].add(-shifted).at[receiver].add(shifted)
    members = jnp.searchsorted(jnp.cumsum(tallies), jnp.arange(rows * top), side="right").astype(jnp.int32)
    table = members.reshape(top, rows).T
    table = table[jax.random.permutation(jax.random.fold_in(own, 1), rows)]
    turn = jax.random.randint(jax.random.fold_in(own, 2), (rows, 1), 0, top)
    return jnp.take_along_axis(table, (jnp.arange(top)[None, :] + turn) % top, axis=1)


def shares(amount, total, reach, slope, full):
    portions = [(1 << 20) // math.isqrt(rank ** slope) + 1 for rank in range(1, amount + 1)]
    largest = reach if full else min(reach, max(-(-total // amount), total * portions[0] // sum(portions)))
    least = 1 if total - largest >= amount - 1 else 0
    counts, rest = [largest] + [least] * (amount - 1), total - largest - least * (amount - 1)
    while rest > 0:
        candidates = [i for i in range(1, amount) if counts[i] < largest] or [i for i in range(1, amount) if counts[i] < reach]
        pool, left = sum([portions[i] for i in candidates]), rest
        for i in candidates:
            more = min(reach - counts[i], max(1, left * portions[i] // pool), rest)
            counts[i] = counts[i] + more
            rest = rest - more
    return np.array(counts)


def gaussian(key, extent, spread, most, cuts=(), kind=jnp.bfloat16):
    entries = jax.random.normal(key, extent, jnp.float32) * spread
    if len(cuts) > 0:
        entries = shard_levels(key, extent, cuts, -0.22, 0.18) * entries
    return jnp.clip(entries, min=-most, max=most).astype(kind)


def setup_inputs(seed: int = 0) -> dict:
    seeds = jax.random.split(jax.random.key(seed), 15)
    queries = gaussian(seeds[0], (SEQUENCE_TOTAL, D), 1.0, 6.0, ((0, 8), (1, 4)))
    forget_pre = draw_forget_pre(jax.random.fold_in(seeds[14], 71), 0)
    value_in = gaussian(seeds[2], (SEQUENCE_TOTAL, D), 1.0, 6.0, ((0, 8), (1, 4)))
    out_gate = gaussian(seeds[3], (SEQUENCE_TOTAL, D), 1.0, 6.0, ((0, 8), (1, 4)))
    lower_bound = jnp.clip(0.5 + 0.3 * jax.random.uniform(seeds[4], (D,), jnp.float32) ** shard_levels(seeds[4], (D,), ((0, 4),), -0.2, 0.2), 0.5, 0.8)
    out_gain = jnp.clip(1.0 + 0.18 * jax.random.normal(seeds[5], (HEAD_DIM,), jnp.float32), 0.1, 1.9)
    out_weight = gaussian(seeds[6], (D, D), D ** -0.5, 0.125, ((0, 4),))
    moe_tokens = gaussian(seeds[7], (MOE_ALL, D), 1.0, 6.0, ((0, 8),))
    moe_gain = jnp.clip(1.0 + 0.18 * jax.random.normal(seeds[8], (D,), jnp.float32), 0.1, 1.9)
    expert_ids_keys = jax.random.split(jax.random.fold_in(seeds[9], 1), MOE_ALL // QROWS)
    expert_ids_turns = jax.random.permutation(jax.random.fold_in(seeds[9], 3), MOE_ALL // QROWS)
    expert_ids = jax.vmap(lambda own, number: deal_out(jax.random.fold_in(seeds[9], 2), own, number, QROWS, EXPERTS, TOPK, CAPQ, 2))(expert_ids_keys, expert_ids_turns).reshape((MOE_ALL, TOPK))
    route_weights = jnp.clip(jnp.exp(math.log(1.0) - 2.3025851 * jax.random.uniform(seeds[10], (MOE_ALL, TOPK), jnp.float32) ** shard_levels(seeds[10], (MOE_ALL, TOPK), ((0, 8),), -0.2, 0.2)), 0.1, 1.0)
    w_gate = gaussian(seeds[11], (EXPERTS, D, FE), D ** -0.5, 0.125, ((0, 8), (2, 4)))
    w_up = gaussian(seeds[12], (EXPERTS, D, FE), D ** -0.5, 0.125, ((0, 8), (2, 4)))
    w_down = gaussian(seeds[13], (EXPERTS, FE, D), FE ** -0.5, 0.1875, ((0, 8), (1, 4)))
    return dict(queries=queries, forget_pre=forget_pre, value_in=value_in, out_gate=out_gate, lower_bound=lower_bound, out_gain=out_gain, out_weight=out_weight, moe_tokens=moe_tokens, moe_gain=moe_gain, expert_ids=expert_ids, route_weights=route_weights, w_gate=w_gate, w_up=w_up, w_down=w_down)


EPS = 1e-06
HIGHEST = lax.Precision.HIGHEST

def rms_scale(values, gain):
    return values * lax.rsqrt(lax.optimization_barrier(jnp.mean(values * values, axis=-1, keepdims=True)) + EPS) * gain

def block_step(memory, inputs):
    queries_block, weight_block, values_block, forget_block = inputs
    cumulative = jnp.cumsum(forget_block, axis=1)
    length = queries_block.shape[1]
    causal = jnp.arange(length, dtype=jnp.int32)[:, None] >= jnp.arange(length, dtype=jnp.int32)[None, :]
    decayed_query = queries_block * jnp.exp(cumulative)
    decayed_key = weight_block * jnp.exp(-cumulative)
    carried_out = jnp.einsum('htd,hde->hte', decayed_query, memory, precision=HIGHEST)
    scores = jnp.einsum('htd,hsd->hts', decayed_query, decayed_key, precision=HIGHEST)
    scores = jnp.where(causal[None], scores, 0.0)
    local_out = jnp.einsum('hts,hse->hte', scores, values_block, precision=HIGHEST)
    block_total = cumulative[:, -1:, :]
    added = jnp.einsum('hsd,hse->hde', weight_block * jnp.exp(block_total - cumulative), values_block, precision=HIGHEST)
    memory = jnp.exp(block_total[:, 0, :])[:, :, None] * memory + added
    return (memory, carried_out + local_out)

def to_blocks(array, head_count):
    row_count = array.shape[0]
    return array.astype(jnp.float32).reshape(row_count // BLOCK, BLOCK, head_count, HEAD_DIM).transpose(0, 2, 1, 3)

def mixer_part(queries, forget_pre, value_in, out_gate, lower_bound, out_gain, out_weight):
    seq_rows, model_width = queries.shape
    head_count = model_width // HEAD_DIM
    weight_in = (1.0 - lower_bound) * jax.nn.sigmoid(-forget_pre)
    log_forget = jnp.log1p(-weight_in)
    start_memory = jnp.zeros((head_count, HEAD_DIM, HEAD_DIM), jnp.float32)
    final_memory, outputs = lax.scan(block_step, start_memory, (to_blocks(queries, head_count), to_blocks(weight_in, head_count), to_blocks(value_in, head_count), to_blocks(log_forget, head_count)))
    outputs = outputs.transpose(0, 2, 1, 3).reshape(seq_rows, head_count, HEAD_DIM)
    gate_act = jax.nn.silu(out_gate.astype(jnp.float32)).reshape(seq_rows, head_count, HEAD_DIM)
    gated = (rms_scale(outputs, out_gain) * gate_act).reshape(seq_rows, model_width).astype(jnp.bfloat16)
    group_width = model_width // N_TP
    summed = jnp.zeros((seq_rows, model_width), jnp.float32)
    for group_index in range(N_TP):
        low = group_index * group_width
        partial_value = jnp.dot(gated[:, low:low + group_width], out_weight[low:low + group_width], preferred_element_type=jnp.float32)
        summed = summed + lax.optimization_barrier(partial_value.astype(jnp.bfloat16)).astype(jnp.float32)
    return summed.astype(jnp.bfloat16)

def slot_ranks(ids_block, expert_count):
    onehot = (ids_block[:, :, None] == jnp.arange(expert_count, dtype=jnp.int32)[None, None, :]).astype(jnp.int32)
    return lax.optimization_barrier(jnp.sum(onehot * (jnp.cumsum(onehot, axis=1) - 1), axis=2)).astype(jnp.int32)

def experts_part(moe_tokens, moe_gain, expert_ids, route_weights, w_gate, w_up, w_down):
    token_count, model_width = moe_tokens.shape
    expert_count = w_gate.shape[0]
    hidden_units = w_gate.shape[2]
    top_count = expert_ids.shape[1]
    normed = rms_scale(moe_tokens.astype(jnp.float32), moe_gain).astype(jnp.bfloat16)
    padded = jnp.concatenate([normed, jnp.zeros((1, model_width), jnp.bfloat16)], axis=0)
    block_count = token_count // QROWS
    ids_block = expert_ids.astype(jnp.int32).reshape(block_count, QROWS * top_count)
    ranks = slot_ranks(ids_block, expert_count)
    block_base = jnp.arange(block_count, dtype=jnp.int32)[:, None] * CAPQ
    columns = (block_base + ranks).reshape(-1)
    flat_ids = ids_block.reshape(-1)
    token_index = jnp.arange(token_count * top_count, dtype=jnp.int32) // top_count
    table = jnp.full((expert_count, block_count * CAPQ), token_count, jnp.int32).at[flat_ids, columns].set(token_index)
    weight_table = jnp.zeros((expert_count, block_count * CAPQ), jnp.float32).at[flat_ids, columns].set(route_weights.reshape(-1))
    group_units = hidden_units // N_TP

    def one_expert(summed, inputs):
        rows_index, weights_now, gate_matrix, up_matrix, down_matrix = inputs
        rows_now = padded[rows_index]
        gate_pre = jnp.dot(rows_now, gate_matrix, preferred_element_type=jnp.float32)
        up_pre = jnp.dot(rows_now, up_matrix, preferred_element_type=jnp.float32)
        hidden = (jax.nn.silu(gate_pre) * up_pre).astype(jnp.bfloat16)
        total_rows = jnp.zeros((rows_now.shape[0], model_width), jnp.float32)
        for group_index in range(N_TP):
            low = group_index * group_units
            partial_value = jnp.dot(hidden[:, low:low + group_units], down_matrix[low:low + group_units], preferred_element_type=jnp.float32)
            total_rows = total_rows + lax.optimization_barrier(partial_value.astype(jnp.bfloat16)).astype(jnp.float32)
        expert_rows = lax.optimization_barrier(total_rows.astype(jnp.bfloat16)).astype(jnp.float32)
        return (summed.at[rows_index].add(expert_rows * weights_now[:, None]), None)
    start_sum = jnp.zeros((token_count + 1, model_width), jnp.float32)
    summed, unused = lax.scan(one_expert, start_sum, (table, weight_table, w_gate, w_up, w_down))
    return summed[:token_count].astype(jnp.bfloat16)

def reference(queries, forget_pre, value_in, out_gate, lower_bound, out_gain, out_weight, moe_tokens, moe_gain, expert_ids, route_weights, w_gate, w_up, w_down):
    mixer_out = mixer_part(queries, forget_pre, value_in, out_gate, lower_bound, out_gain, out_weight)
    expert_out = experts_part(moe_tokens, moe_gain, expert_ids, route_weights, w_gate, w_up, w_down)
    return (mixer_out, expert_out)
```

```python
import jax
import jax.numpy as jnp
from jax import lax
from jax.experimental import pallas as pl
from jax.experimental.pallas import tpu as pltpu
from jax.sharding import PartitionSpec as P

HEAD_DIM = 128
BLOCK = 64


EPS = 1e-06
HIGHEST = lax.Precision.HIGHEST


def rms_scale(values, gain):
    return values * lax.rsqrt(jnp.mean(values * values, axis=-1, keepdims=True) + EPS) * gain


def block_step(memory, inputs):
    queries_block, weight_block, values_block, forget_block = inputs
    cumulative = jnp.cumsum(forget_block, axis=1)
    length = queries_block.shape[1]
    causal = (
        jnp.arange(length, dtype=jnp.int32)[:, None] >= jnp.arange(length, dtype=jnp.int32)[None, :]
    )
    decayed_query = queries_block * jnp.exp(cumulative)
    decayed_key = weight_block * jnp.exp(-cumulative)
    carried_out = jnp.einsum("htd,hde->hte", decayed_query, memory, precision=HIGHEST)
    scores = jnp.einsum("htd,hsd->hts", decayed_query, decayed_key, precision=HIGHEST)
    scores = jnp.where(causal[None], scores, 0.0)
    local_out = jnp.einsum("hts,hse->hte", scores, values_block, precision=HIGHEST)
    block_total = cumulative[:, -1:, :]
    added = jnp.einsum(
        "hsd,hse->hde",
        weight_block * jnp.exp(block_total - cumulative),
        values_block,
        precision=HIGHEST,
    )
    memory = jnp.exp(block_total[:, 0, :])[:, :, None] * memory + added
    return (memory, carried_out + local_out)


def to_blocks(array, head_count):
    row_count = array.shape[0]
    return (
        array.astype(jnp.float32)
        .reshape(row_count // BLOCK, BLOCK, head_count, HEAD_DIM)
        .transpose(0, 2, 1, 3)
    )


def slot_ranks(ids_block, expert_count):
    onehot = (
        ids_block[:, :, None] == jnp.arange(expert_count, dtype=jnp.int32)[None, None, :]
    ).astype(jnp.int32)
    return jnp.sum(onehot * (jnp.cumsum(onehot, axis=1) - 1), axis=2)


MESH = pl.DeviceIdType.MESH
VMEM = pl.BlockSpec(memory_space=pltpu.VMEM)


def ring_place(index, planes):
    plane, side = index // 2, index % 2
    return (1 - side) * plane + side * (2 * planes - 1 - plane)


def ring_index(place, planes):
    back = place // planes
    return (1 - back) * 2 * place + back * ((2 * planes - 1 - place) * 2 + 1)


def ring_setup(count):
    planes = count // 2
    index = lax.axis_index("ep")
    lane = lax.axis_index("tp")
    place = ring_place(index, planes)
    right = ring_index((place + 1) % count, planes)
    left = ring_index((place + count - 1) % count, planes)
    core = lane % 2
    partner = lane + 1 - 2 * core
    return index, lane, core, (right, lane), (left, lane), (index, partner)


def greet(devices):
    barrier = pltpu.get_barrier_semaphore()
    for device in devices:
        pl.semaphore_signal(barrier, inc=1, device_id=device, device_id_type=MESH)
    pl.semaphore_wait(barrier, len(devices))


def remote(source, target, send, receive, device):
    return pltpu.make_async_remote_copy(
        src_ref=source,
        dst_ref=target,
        send_sem=send,
        recv_sem=receive,
        device_id=device,
        device_id_type=MESH,
    )


def gather_kernel(
    count, experts, width, own_ref, gate_ref, up_ref, down_ref, out_ref, held, send, recv, psend, precv
):
    index, lane, core, right, left, partner = ring_setup(count)
    local_experts = gate_ref.shape[0]
    half = held.shape[2]
    turns = count // 2
    greet((right, left, partner))

    def part(side, turn):
        if turn < turns:
            return pl.ds(0, half)
        return pl.ds(side * (half // 2), half // 2)

    def slot(side, turn):
        return turn if side == 0 else count - turn

    def hop(side, turn):
        rows = part(side, turn)
        target = held.at[slot(side, turn), core, rows]
        source = (
            own_ref.at[core, rows] if turn == 1 else held.at[slot(side, turn - 1), core, rows]
        )
        return remote(
            source, target, send.at[side, turn - 1], recv.at[side, turn - 1], (right, left)[side]
        )

    def across(side, turn):
        piece = held.at[slot(side, turn), core, part(side, turn)]
        return remote(piece, piece, psend.at[side, turn - 1], precv.at[side, turn - 1], partner)

    def landed(side, turn):
        piece = held.at[slot(side, turn), 1 - core, part(side, turn)]
        return remote(piece, piece, psend.at[side, turn - 1], precv.at[side, turn - 1], partner)

    def experts_of(block, place):
        rows = block.shape[0]
        tokens = block[:, :width]
        extra = block[:, width:].astype(jnp.float32)
        column = lax.broadcasted_iota(jnp.int32, extra.shape, 1)
        hidden = []
        for expert in range(local_experts):
            number = index * local_experts + expert
            chosen = (column == number) | (column == number + experts)
            weight = jnp.sum(jnp.where(chosen, extra, 0.0), axis=1, keepdims=True)
            gate = jnp.dot(tokens, gate_ref[expert], preferred_element_type=jnp.float32)
            up = jnp.dot(tokens, up_ref[expert], preferred_element_type=jnp.float32)
            hidden.append((jax.nn.silu(gate) * up * weight).astype(jnp.bfloat16))
        total = jnp.dot(hidden[0], down_ref[0], preferred_element_type=jnp.float32)
        for expert in range(1, local_experts):
            total += jnp.dot(
                hidden[expert], down_ref[expert], preferred_element_type=jnp.float32
            )
        for part_at in range(2):
            out_ref[place, part_at] = total[part_at * half : (part_at + 1) * half].astype(
                jnp.bfloat16
            )

    for side in range(2):
        hop(side, 1).start()
    experts_of(own_ref[...].reshape(2 * half, own_ref.shape[2]), 0)
    for turn in range(1, turns + 1):
        for side in range(2):
            hop(side, turn).wait_recv()
            if turn < turns:
                hop(side, turn + 1).start()
            across(side, turn).start()
        for side in range(2):
            landed(side, turn).wait_recv()
        if turn < turns:

            def body(step, carry):
                place = turn + step * (count - 2 * turn)
                experts_of(held[place].reshape(2 * half, held.shape[3]), place)
                return carry

            lax.fori_loop(0, 2, body, 0)
        else:
            experts_of(held[turn].reshape(2 * half, held.shape[3]), turn)
    for turn in range(1, turns + 1):
        for side in range(2):
            hop(side, turn).wait_send()
            across(side, turn).wait_send()


def scatter_kernel(
    count, part_ref, out_ref, total, other, came, final, crossed, send, recv, psend, precv, xsend, xrecv
):
    index, lane, core, right, left, partner = ring_setup(count)
    half = part_ref.shape[2]
    turns = count // 2
    cross_at = lane // 2
    cross = (index, lane + 2 - 4 * cross_at)
    greet((right, left, partner, cross))
    order = [turns]
    for distance in range(turns - 1, 0, -1):
        order += [count - distance, distance]
    order += [0]

    def swap(place):
        return remote(
            part_ref.at[place, 1 - core], other.at[place], psend.at[place], precv.at[place], partner
        )

    for place in order:
        swap(place).start()

    def settle(place):
        swap(place).wait_recv()
        total[place] = (
            part_ref[place, core].astype(jnp.float32) + other[place].astype(jnp.float32)
        ).astype(jnp.bfloat16)

    def rows_of(side, turn):
        if turn > 1:
            return pl.ds(0, half)
        return pl.ds(side * (half // 2), half // 2)

    def hop(side, turn):
        distance = turns - turn + 1
        place = count - distance if side == 0 else distance
        rows = rows_of(side, turn)
        return remote(
            total.at[place, rows],
            came.at[side, turn - 1, rows],
            send.at[side, turn - 1],
            recv.at[side, turn - 1],
            (right, left)[side],
        )

    settle(turns)
    for side in range(2):
        hop(side, 1).start()
    for turn in range(1, turns):
        distance = turns - turn
        for side in range(2):
            settle(count - distance if side == 0 else distance)
        for side in range(2):
            place = count - distance if side == 0 else distance
            rows = rows_of(side, turn)
            hop(side, turn).wait_recv()
            total[place, rows] = (
                total[place, rows].astype(jnp.float32)
                + came[side, turn - 1, rows].astype(jnp.float32)
            ).astype(jnp.bfloat16)
            hop(side, turn + 1).start()
    swap(0).wait_recv()
    for side in range(2):
        hop(side, turns).wait_recv()
    summed = (
        part_ref[0, core].astype(jnp.float32)
        + other[0].astype(jnp.float32)
        + came[0, turns - 1].astype(jnp.float32)
        + came[1, turns - 1].astype(jnp.float32)
    )
    final[...] = summed.astype(jnp.bfloat16).reshape(final.shape)
    over = remote(final.at[1 - cross_at], crossed, xsend, xrecv, cross)
    over.start()
    over.wait_recv()
    out_ref[...] = (final[cross_at].astype(jnp.float32) + crossed[...].astype(jnp.float32)).astype(
        jnp.bfloat16
    )
    over.wait_send()
    for place in range(count):
        swap(place).wait_send()
    for turn in range(1, turns + 1):
        for side in range(2):
            hop(side, turn).wait_send()


def dense_parts(normed, ids, weights, w_gate, w_up, w_down, ep_count):
    rows, width = normed.shape
    local_experts = w_gate.shape[0]
    experts = local_experts * ep_count
    half = rows // 2
    routes = jnp.sum(
        jnp.where(
            ids[:, :, None] == jnp.arange(experts, dtype=jnp.int32)[None, None, :],
            weights[:, :, None],
            0.0,
        ),
        axis=1,
    )
    high = lax.reduce_precision(routes, 8, 7)
    low = routes - high
    margin = -(-2 * experts // 128) * 128
    extra = jnp.concatenate(
        [high, low, jnp.zeros((rows, margin - 2 * experts), jnp.float32)], axis=1
    ).astype(jnp.bfloat16)
    full = jnp.concatenate([normed, extra], axis=1)
    stride = width + margin
    full = full.reshape(2, 2, half // 2, stride).transpose(1, 0, 2, 3).reshape(2, half, stride)
    turns = ep_count // 2
    return full, margin, half, turns, experts


def moe_gather(full, w_gate, w_up, w_down, ep_count, experts):
    half, stride = full.shape[1:]
    width = w_down.shape[2]
    turns = ep_count // 2
    sems = pltpu.SemaphoreType.DMA((2, turns))
    rows = 2 * half * ep_count
    flops = 2 * rows * w_gate.size * 3
    return pl.pallas_call(
        lambda *refs: gather_kernel(ep_count, experts, width, *refs),
        out_shape=jax.ShapeDtypeStruct((ep_count, 2, half, width), jnp.bfloat16),
        in_specs=[VMEM] * 4,
        out_specs=VMEM,
        scratch_shapes=[
            pltpu.VMEM((ep_count, 2, half, stride), jnp.bfloat16),
            sems,
            sems,
            sems,
            sems,
        ],
        compiler_params=pltpu.CompilerParams(
            collective_id=0, has_side_effects=True, vmem_limit_bytes=58 * 2**20
        ),
        cost_estimate=pl.CostEstimate(
            flops=flops, bytes_accessed=100 * 2**20, transcendentals=0
        ),
        name="moe_gather",
    )(full, w_gate, w_up, w_down)


def moe_scatter(parts):
    count, _, half, width = parts.shape
    turns = count // 2
    sems = pltpu.SemaphoreType.DMA((2, turns))
    each = pltpu.SemaphoreType.DMA((count,))
    block = (count, half, width)
    return pl.pallas_call(
        lambda *refs: scatter_kernel(count, *refs),
        out_shape=jax.ShapeDtypeStruct((half // 2, width), jnp.bfloat16),
        in_specs=[VMEM],
        out_specs=VMEM,
        scratch_shapes=[
            pltpu.VMEM(block, jnp.bfloat16),
            pltpu.VMEM(block, jnp.bfloat16),
            pltpu.VMEM((2, turns, half, width), jnp.bfloat16),
            pltpu.VMEM((2, half // 2, width), jnp.bfloat16),
            pltpu.VMEM((half // 2, width), jnp.bfloat16),
            sems,
            sems,
            each,
            each,
            pltpu.SemaphoreType.DMA,
            pltpu.SemaphoreType.DMA,
        ],
        compiler_params=pltpu.CompilerParams(
            collective_id=1, has_side_effects=True, vmem_limit_bytes=58 * 2**20
        ),
        cost_estimate=pl.CostEstimate(
            flops=0, bytes_accessed=150 * 2**20, transcendentals=0
        ),
        name="moe_scatter",
    )(parts)


def sparse_experts(
    moe_tokens, moe_gain, expert_ids, route_weights, w_gate, w_up, w_down, model_width
):
    lanes = lax.axis_size("tp")
    lane_index = lax.axis_index("tp")
    ep_count = lax.axis_size("ep")
    qrows = moe_tokens.shape[0] // lanes
    top_count = expert_ids.shape[1]
    local_experts = w_gate.shape[0]
    expert_count = local_experts * ep_count
    capacity = max(2, 2 * qrows * top_count // expert_count)
    send_tokens = lax.dynamic_slice_in_dim(moe_tokens, lane_index * qrows, qrows, 0)
    send_ids = lax.dynamic_slice_in_dim(expert_ids, lane_index * qrows, qrows, 0)
    quarters = send_tokens.shape[0] // qrows
    normed = rms_scale(send_tokens.astype(jnp.float32), moe_gain).astype(jnp.bfloat16)
    ids_block = send_ids.reshape(quarters, qrows * top_count)
    ranks = slot_ranks(ids_block, expert_count)
    quarter_base = jnp.arange(quarters, dtype=jnp.int32)[:, None] * (expert_count * capacity)
    slot_index = (quarter_base + ids_block * capacity + ranks).reshape(-1)
    source_row = jnp.arange(quarters * qrows * top_count, dtype=jnp.int32) // top_count
    sources = (
        jnp.full((quarters * expert_count * capacity,), quarters * qrows, jnp.int32)
        .at[slot_index]
        .set(source_row)
    )
    padded = jnp.concatenate([normed, jnp.zeros((1, model_width), jnp.bfloat16)], axis=0)
    outgoing = padded[sources].reshape(quarters, ep_count, local_experts * capacity, model_width)
    arrived = lax.all_to_all(outgoing, "ep", split_axis=1, concat_axis=1, tiled=True)
    piece = lax.all_gather(arrived, "tp", axis=0, tiled=True)
    shaped = piece.reshape(piece.shape[0], ep_count, local_experts, capacity, model_width)
    gate_pre = jnp.einsum("qsecd,edf->qsecf", shaped, w_gate, preferred_element_type=jnp.float32)
    up_pre = jnp.einsum("qsecd,edf->qsecf", shaped, w_up, preferred_element_type=jnp.float32)
    hidden = (jax.nn.silu(gate_pre) * up_pre).astype(jnp.bfloat16)
    lane_rows = ep_count * local_experts * capacity
    projected = jnp.einsum("qsecf,efd->qsecd", hidden, w_down, preferred_element_type=jnp.float32)
    expert_sum = lax.psum_scatter(
        projected.reshape(lax.axis_size("tp") * lane_rows, model_width).astype(jnp.bfloat16),
        "tp",
        scatter_dimension=0,
        tiled=True,
    )
    leaving = expert_sum.reshape(ep_count, local_experts * capacity, model_width)
    returned = lax.all_to_all(leaving, "ep", split_axis=0, concat_axis=0, tiled=True)
    returned = returned.reshape(expert_count * capacity, model_width)
    own_quarter = lane_index * (quarters // lanes)
    own_ids = lax.dynamic_index_in_dim(ids_block, own_quarter, 0, keepdims=False)
    own_ranks = lax.dynamic_index_in_dim(ranks, own_quarter, 0, keepdims=False)
    picked = (
        returned[own_ids * capacity + own_ranks]
        .astype(jnp.float32)
        .reshape(qrows, top_count, model_width)
    )
    own_weights = lax.dynamic_slice_in_dim(route_weights, lane_index * qrows, qrows, 0)
    expert_out = jnp.sum(picked * own_weights[:, :, None], axis=1).astype(jnp.bfloat16)
    return expert_out


def local(
    queries,
    forget_pre,
    value_in,
    out_gate,
    lower_bound,
    out_gain,
    out_weight,
    moe_tokens,
    moe_gain,
    expert_ids,
    route_weights,
    w_gate,
    w_up,
    w_down,
):
    lanes = lax.axis_size("tp")
    ep_count = lax.axis_size("ep")
    seq_rows, local_width = queries.shape
    model_width = out_weight.shape[1]
    head_count = local_width // HEAD_DIM
    weight_in = (1.0 - lower_bound) * jax.nn.sigmoid(-forget_pre)
    log_forget = jnp.log1p(-weight_in)
    cumulative = jnp.cumsum(log_forget, axis=0)
    span_total = cumulative[-1]
    to_end = (weight_in * jnp.exp(span_total[None, :] - cumulative)).reshape(
        seq_rows, head_count, HEAD_DIM
    )
    values_float = value_in.astype(jnp.float32).reshape(seq_rows, head_count, HEAD_DIM)
    local_memory = jnp.einsum("shd,she->hde", to_end, values_float, precision=HIGHEST)
    decay_total = jnp.exp(span_total).reshape(head_count, HEAD_DIM)
    packed = jnp.concatenate([local_memory, decay_total[:, None, :]], axis=1)
    tokens, top_count = expert_ids.shape
    dense_slots = 2 * (tokens // lanes) * top_count * lanes
    dense = lanes == 4 and ep_count % 2 == 0 and tokens * ep_count <= dense_slots
    if dense:
        normed = rms_scale(moe_tokens.astype(jnp.float32), moe_gain).astype(jnp.bfloat16)
        full, _, _, _, experts = dense_parts(
            normed, expert_ids, route_weights, w_gate, w_up, w_down, ep_count
        )
        full, packed = lax.optimization_barrier((full, packed))
    gathered = lax.all_gather(packed, "ep")
    if dense:
        parts = moe_gather(full, w_gate, w_up, w_down, ep_count, experts)
        gathered, parts = lax.optimization_barrier((gathered, parts))
    place = lax.axis_index("ep")

    def one(hop, state):
        block = lax.dynamic_index_in_dim(gathered, hop, 0, False)
        return block[:, HEAD_DIM:, :].reshape(head_count, HEAD_DIM, 1) * state + block[:, :HEAD_DIM]

    earlier_memory = lax.fori_loop(0, place, one, jnp.zeros_like(local_memory))
    final_memory, outputs = lax.scan(
        block_step,
        earlier_memory,
        (
            to_blocks(queries, head_count),
            to_blocks(weight_in, head_count),
            to_blocks(value_in, head_count),
            to_blocks(log_forget, head_count),
        ),
    )
    outputs = outputs.transpose(0, 2, 1, 3).reshape(seq_rows, head_count, HEAD_DIM)
    gate_act = jax.nn.silu(out_gate.astype(jnp.float32)).reshape(seq_rows, head_count, HEAD_DIM)
    gated = (
        (rms_scale(outputs, out_gain) * gate_act)
        .reshape(seq_rows, local_width)
        .astype(jnp.bfloat16)
    )
    mixer_part = jnp.dot(gated, out_weight, preferred_element_type=jnp.float32).astype(
        jnp.bfloat16
    )
    if dense:
        mixer_part, parts = lax.optimization_barrier((mixer_part, parts))
    mixer_sum = lax.psum_scatter(mixer_part, "tp", scatter_dimension=0, tiled=True)
    if dense:
        expert_out = moe_scatter(parts)
    else:
        expert_out = sparse_experts(
            moe_tokens, moe_gain, expert_ids, route_weights, w_gate, w_up, w_down, model_width
        )
    return (mixer_sum, expert_out)


def solution(mesh):
    in_specs = (
        P("ep", "tp"),
        P("ep", "tp"),
        P("ep", "tp"),
        P("ep", "tp"),
        P("tp"),
        P(),
        P("tp", None),
        P("ep", None),
        P(),
        P("ep", None),
        P("ep", None),
        P("ep", None, "tp"),
        P("ep", None, "tp"),
        P("ep", "tp", None),
    )
    out_specs = (P(("ep", "tp"), None), P(("ep", "tp"), None))
    return jax.shard_map(local, mesh=mesh, in_specs=in_specs, out_specs=out_specs, check_vma=False)
```

```python
import jax
import jax.numpy as jnp
from jax import lax
from jax.experimental import pallas as pl
from jax.experimental.pallas import tpu as pltpu
from jax.sharding import PartitionSpec as P

HEAD_DIM = 128
BLOCK = 64


EPS = 1e-06
HIGHEST = lax.Precision.HIGHEST


def rms_scale(values, gain):
    return values * lax.rsqrt(jnp.mean(values * values, axis=-1, keepdims=True) + EPS) * gain


def slot_ranks(ids_block, expert_count):
    onehot = (
        ids_block[:, :, None] == jnp.arange(expert_count, dtype=jnp.int32)[None, None, :]
    ).astype(jnp.int32)
    return jnp.sum(onehot * (jnp.cumsum(onehot, axis=1) - 1), axis=2)


MESH = pl.DeviceIdType.MESH
VMEM = pl.BlockSpec(memory_space=pltpu.VMEM)


def ring_place(index, planes):
    plane, side = index // 2, index % 2
    return (1 - side) * plane + side * (2 * planes - 1 - plane)


def ring_index(place, planes):
    back = place // planes
    return (1 - back) * 2 * place + back * ((2 * planes - 1 - place) * 2 + 1)


def ring_setup(count):
    planes = count // 2
    index = lax.axis_index("ep")
    lane = lax.axis_index("tp")
    place = ring_place(index, planes)
    right = ring_index((place + 1) % count, planes)
    left = ring_index((place + count - 1) % count, planes)
    core = lane % 2
    partner = lane + 1 - 2 * core
    return index, lane, core, (right, lane), (left, lane), (index, partner)


def greet(devices):
    barrier = pltpu.get_barrier_semaphore()
    for device in devices:
        pl.semaphore_signal(barrier, inc=1, device_id=device, device_id_type=MESH)
    pl.semaphore_wait(barrier, len(devices))


def remote(source, target, send, receive, device):
    return pltpu.make_async_remote_copy(
        src_ref=source,
        dst_ref=target,
        send_sem=send,
        recv_sem=receive,
        device_id=device,
        device_id_type=MESH,
    )


def gather_kernel(
    count, experts, width, own_ref, gate_ref, up_ref, down_ref, out_ref, held, send, recv, psend, precv
):
    index, lane, core, right, left, partner = ring_setup(count)
    local_experts = gate_ref.shape[0]
    half = held.shape[2]
    turns = count // 2
    greet((right, left, partner))

    def part(side, turn):
        if turn < turns:
            return pl.ds(0, half)
        return pl.ds(side * (half // 2), half // 2)

    def slot(side, turn):
        return turn if side == 0 else count - turn

    def hop(side, turn):
        rows = part(side, turn)
        target = held.at[slot(side, turn), core, rows]
        source = (
            own_ref.at[core, rows] if turn == 1 else held.at[slot(side, turn - 1), core, rows]
        )
        return remote(
            source, target, send.at[side, turn - 1], recv.at[side, turn - 1], (right, left)[side]
        )

    def across(side, turn):
        piece = held.at[slot(side, turn), core, part(side, turn)]
        return remote(piece, piece, psend.at[side, turn - 1], precv.at[side, turn - 1], partner)

    def landed(side, turn):
        piece = held.at[slot(side, turn), 1 - core, part(side, turn)]
        return remote(piece, piece, psend.at[side, turn - 1], precv.at[side, turn - 1], partner)

    def experts_of(block, place):
        rows = block.shape[0]
        tokens = block[:, :width]
        extra = block[:, width:].astype(jnp.float32)
        column = lax.broadcasted_iota(jnp.int32, extra.shape, 1)
        hidden = []
        for expert in range(local_experts):
            number = index * local_experts + expert
            chosen = (column == number) | (column == number + experts)
            weight = jnp.sum(jnp.where(chosen, extra, 0.0), axis=1, keepdims=True)
            gate = jnp.dot(tokens, gate_ref[expert], preferred_element_type=jnp.float32)
            up = jnp.dot(tokens, up_ref[expert], preferred_element_type=jnp.float32)
            hidden.append((jax.nn.silu(gate) * up * weight).astype(jnp.bfloat16))
        total = jnp.dot(hidden[0], down_ref[0], preferred_element_type=jnp.float32)
        for expert in range(1, local_experts):
            total += jnp.dot(
                hidden[expert], down_ref[expert], preferred_element_type=jnp.float32
            )
        for part_at in range(2):
            out_ref[place, part_at] = total[part_at * half : (part_at + 1) * half].astype(
                jnp.bfloat16
            )

    for side in range(2):
        hop(side, 1).start()
    experts_of(own_ref[...].reshape(2 * half, own_ref.shape[2]), 0)
    for turn in range(1, turns + 1):
        for side in range(2):
            hop(side, turn).wait_recv()
            if turn < turns:
                hop(side, turn + 1).start()
            across(side, turn).start()
        for side in range(2):
            landed(side, turn).wait_recv()
        if turn < turns:

            def body(step, carry):
                place = turn + step * (count - 2 * turn)
                experts_of(held[place].reshape(2 * half, held.shape[3]), place)
                return carry

            lax.fori_loop(0, 2, body, 0)
        else:
            experts_of(held[turn].reshape(2 * half, held.shape[3]), turn)
    for turn in range(1, turns + 1):
        for side in range(2):
            hop(side, turn).wait_send()
            across(side, turn).wait_send()


def scatter_kernel(
    count, part_ref, out_ref, total, other, came, final, crossed, send, recv, psend, precv, xsend, xrecv
):
    index, lane, core, right, left, partner = ring_setup(count)
    half = part_ref.shape[2]
    turns = count // 2
    cross_at = lane // 2
    cross = (index, lane + 2 - 4 * cross_at)
    greet((right, left, partner, cross))
    order = [turns]
    for distance in range(turns - 1, 0, -1):
        order += [count - distance, distance]
    order += [0]

    def swap(place):
        return remote(
            part_ref.at[place, 1 - core], other.at[place], psend.at[place], precv.at[place], partner
        )

    for place in order:
        swap(place).start()

    def settle(place):
        swap(place).wait_recv()
        total[place] = (
            part_ref[place, core].astype(jnp.float32) + other[place].astype(jnp.float32)
        ).astype(jnp.bfloat16)

    def rows_of(side, turn):
        if turn > 1:
            return pl.ds(0, half)
        return pl.ds(side * (half // 2), half // 2)

    def hop(side, turn):
        distance = turns - turn + 1
        place = count - distance if side == 0 else distance
        rows = rows_of(side, turn)
        return remote(
            total.at[place, rows],
            came.at[side, turn - 1, rows],
            send.at[side, turn - 1],
            recv.at[side, turn - 1],
            (right, left)[side],
        )

    settle(turns)
    for side in range(2):
        hop(side, 1).start()
    for turn in range(1, turns):
        distance = turns - turn
        for side in range(2):
            settle(count - distance if side == 0 else distance)
        for side in range(2):
            place = count - distance if side == 0 else distance
            rows = rows_of(side, turn)
            hop(side, turn).wait_recv()
            total[place, rows] = (
                total[place, rows].astype(jnp.float32)
                + came[side, turn - 1, rows].astype(jnp.float32)
            ).astype(jnp.bfloat16)
            hop(side, turn + 1).start()
    swap(0).wait_recv()
    for side in range(2):
        hop(side, turns).wait_recv()
    summed = (
        part_ref[0, core].astype(jnp.float32)
        + other[0].astype(jnp.float32)
        + came[0, turns - 1].astype(jnp.float32)
        + came[1, turns - 1].astype(jnp.float32)
    )
    final[...] = summed.astype(jnp.bfloat16).reshape(final.shape)
    over = remote(final.at[1 - cross_at], crossed, xsend, xrecv, cross)
    over.start()
    over.wait_recv()
    out_ref[...] = (final[cross_at].astype(jnp.float32) + crossed[...].astype(jnp.float32)).astype(
        jnp.bfloat16
    )
    over.wait_send()
    for place in range(count):
        swap(place).wait_send()
    for turn in range(1, turns + 1):
        for side in range(2):
            hop(side, turn).wait_send()


def contract(left, right, left_dim, right_dim):
    return lax.dot_general(
        left,
        right,
        (((left_dim,), (right_dim,)), ((), ())),
        precision=HIGHEST,
        preferred_element_type=jnp.float32,
    )


def decay_blocks(forget, bound):
    weight = (1.0 - bound) * jax.nn.sigmoid(-forget)
    logs = jnp.log1p(-weight)
    lower = (
        lax.broadcasted_iota(jnp.int32, (BLOCK, BLOCK), 0)
        >= lax.broadcasted_iota(jnp.int32, (BLOCK, BLOCK), 1)
    )
    ones = jnp.where(lower, 1.0, 0.0)
    blocks = []
    for low in range(0, forget.shape[0], BLOCK):
        cumulative = contract(ones, logs[low : low + BLOCK], 1, 0)
        total = cumulative[BLOCK - 1 :]
        blocks.append((weight[low : low + BLOCK], cumulative, total))
    return lower, blocks


def state_kernel(forget_ref, value_ref, bound_ref, out_ref):
    _, blocks = decay_blocks(forget_ref[...], bound_ref[...])
    memory, span = None, None
    for at, (weight, cumulative, total) in enumerate(blocks):
        values = value_ref[at * BLOCK : (at + 1) * BLOCK].astype(jnp.float32)
        added = contract(values, weight * jnp.exp(total - cumulative), 0, 0)
        memory = added if memory is None else memory * jnp.exp(total) + added
        span = total if span is None else span + total
    decay = jnp.broadcast_to(jnp.exp(span), (16, HEAD_DIM))
    high = decay.astype(jnp.bfloat16).astype(jnp.float32)
    first = lax.broadcasted_iota(jnp.int32, decay.shape, 0) < 8
    out_ref[0, :HEAD_DIM] = memory.astype(jnp.bfloat16)
    out_ref[0, HEAD_DIM:] = jnp.where(first, high, decay - high).astype(jnp.bfloat16)


def mixer_kernel(
    states_ref, query_ref, forget_ref, value_ref, gate_ref, bound_ref, gain_ref, out_ref
):
    def one(hop, memory):
        tail = states_ref[hop, 0, HEAD_DIM:].astype(jnp.float32)
        return memory * (tail[0:1] + tail[8:9]) + states_ref[hop, 0, :HEAD_DIM].astype(jnp.float32)

    memory = lax.fori_loop(
        0, lax.axis_index("ep"), one, jnp.zeros((HEAD_DIM, HEAD_DIM), jnp.float32)
    )
    lower, blocks = decay_blocks(forget_ref[...], bound_ref[...])
    for at, (weight, cumulative, total) in enumerate(blocks):
        rows = slice(at * BLOCK, (at + 1) * BLOCK)
        values = value_ref[rows].astype(jnp.float32)
        decayed_query = query_ref[rows].astype(jnp.float32) * jnp.exp(cumulative)
        scores = contract(decayed_query, weight * jnp.exp(-cumulative), 1, 1)
        result = contract(jnp.where(lower, scores, 0.0), values, 1, 0)
        result += contract(decayed_query, memory, 1, 1)
        added = contract(values, weight * jnp.exp(total - cumulative), 0, 0)
        memory = memory * jnp.exp(total) + added
        gate = jax.nn.silu(gate_ref[rows].astype(jnp.float32))
        out_ref[rows] = (rms_scale(result, gain_ref[...]) * gate).astype(jnp.bfloat16)


def head_block(rows):
    return pl.BlockSpec((rows, HEAD_DIM), lambda head: (0, head))


def head_states(forget_pre, value_in, lower_bound):
    rows, width = forget_pre.shape
    heads = width // HEAD_DIM
    return pl.pallas_call(
        state_kernel,
        grid=(heads,),
        out_shape=jax.ShapeDtypeStruct((heads, HEAD_DIM + 16, HEAD_DIM), jnp.bfloat16),
        in_specs=[head_block(rows), head_block(rows), head_block(1)],
        out_specs=pl.BlockSpec((1, HEAD_DIM + 16, HEAD_DIM), lambda head: (head, 0, 0)),
        cost_estimate=pl.CostEstimate(
            flops=10**9, bytes_accessed=8 * forget_pre.size, transcendentals=0
        ),
        name="head_states",
    )(forget_pre, value_in, lower_bound[None])


def mix_heads(states, queries, forget_pre, value_in, out_gate, lower_bound, out_gain):
    rows, width = forget_pre.shape
    heads = width // HEAD_DIM
    count = states.shape[0]
    return pl.pallas_call(
        mixer_kernel,
        grid=(heads,),
        out_shape=jax.ShapeDtypeStruct((rows, width), jnp.bfloat16),
        in_specs=[
            pl.BlockSpec((count, 1, HEAD_DIM + 16, HEAD_DIM), lambda head: (0, head, 0, 0)),
            head_block(rows),
            head_block(rows),
            head_block(rows),
            head_block(rows),
            head_block(1),
            pl.BlockSpec((1, HEAD_DIM), lambda head: (0, 0)),
        ],
        out_specs=head_block(rows),
        cost_estimate=pl.CostEstimate(
            flops=4 * 10**9, bytes_accessed=16 * forget_pre.size, transcendentals=0
        ),
        name="mix_heads",
    )(states, queries, forget_pre, value_in, out_gate, lower_bound[None], out_gain[None])


def prepare_kernel(experts, token_ref, gain_ref, ids_ref, weights_ref, out_ref):
    rows, width = token_ref.shape
    normed = rms_scale(token_ref[...].astype(jnp.float32), gain_ref[...]).astype(jnp.bfloat16)
    margin = out_ref.shape[2] - width
    column = lax.broadcasted_iota(jnp.int32, (rows, margin), 1)
    extra = jnp.zeros((rows, margin), jnp.float32)
    for choice in range(ids_ref.shape[1]):
        number = ids_ref[:, choice : choice + 1]
        weight = weights_ref[:, choice : choice + 1]
        high = weight.astype(jnp.bfloat16).astype(jnp.float32)
        extra += jnp.where(column == number, high, 0.0)
        extra += jnp.where(column == number + experts, weight - high, 0.0)
    extra = extra.astype(jnp.bfloat16)
    step = rows // 4
    for core in range(2):
        for cross in range(2):
            low = (2 * cross + core) * step
            out_ref[core, cross * step : (cross + 1) * step, :width] = normed[low : low + step]
            out_ref[core, cross * step : (cross + 1) * step, width:] = extra[low : low + step]


def prepare(tokens, gain, ids, weights, experts):
    rows, width = tokens.shape
    margin = -(-2 * experts // 128) * 128
    return pl.pallas_call(
        lambda *refs: prepare_kernel(experts, *refs),
        out_shape=jax.ShapeDtypeStruct((2, rows // 2, width + margin), jnp.bfloat16),
        in_specs=[VMEM] * 4,
        out_specs=VMEM,
        cost_estimate=pl.CostEstimate(
            flops=10**6, bytes_accessed=4 * tokens.size, transcendentals=0
        ),
        name="prepare",
    )(tokens, gain[None], ids, weights)


def moe_gather(full, w_gate, w_up, w_down, ep_count, experts):
    half, stride = full.shape[1:]
    width = w_down.shape[2]
    turns = ep_count // 2
    sems = pltpu.SemaphoreType.DMA((2, turns))
    rows = 2 * half * ep_count
    flops = 2 * rows * w_gate.size * 3
    return pl.pallas_call(
        lambda *refs: gather_kernel(ep_count, experts, width, *refs),
        out_shape=jax.ShapeDtypeStruct((ep_count, 2, half, width), jnp.bfloat16),
        in_specs=[VMEM] * 4,
        out_specs=VMEM,
        scratch_shapes=[
            pltpu.VMEM((ep_count, 2, half, stride), jnp.bfloat16),
            sems,
            sems,
            sems,
            sems,
        ],
        compiler_params=pltpu.CompilerParams(
            collective_id=0, has_side_effects=True, vmem_limit_bytes=58 * 2**20
        ),
        cost_estimate=pl.CostEstimate(
            flops=flops, bytes_accessed=100 * 2**20, transcendentals=0
        ),
        name="moe_gather",
    )(full, w_gate, w_up, w_down)


def moe_scatter(parts):
    count, _, half, width = parts.shape
    turns = count // 2
    sems = pltpu.SemaphoreType.DMA((2, turns))
    each = pltpu.SemaphoreType.DMA((count,))
    block = (count, half, width)
    return pl.pallas_call(
        lambda *refs: scatter_kernel(count, *refs),
        out_shape=jax.ShapeDtypeStruct((half // 2, width), jnp.bfloat16),
        in_specs=[VMEM],
        out_specs=VMEM,
        scratch_shapes=[
            pltpu.VMEM(block, jnp.bfloat16),
            pltpu.VMEM(block, jnp.bfloat16),
            pltpu.VMEM((2, turns, half, width), jnp.bfloat16),
            pltpu.VMEM((2, half // 2, width), jnp.bfloat16),
            pltpu.VMEM((half // 2, width), jnp.bfloat16),
            sems,
            sems,
            each,
            each,
            pltpu.SemaphoreType.DMA,
            pltpu.SemaphoreType.DMA,
        ],
        compiler_params=pltpu.CompilerParams(
            collective_id=1, has_side_effects=True, vmem_limit_bytes=58 * 2**20
        ),
        cost_estimate=pl.CostEstimate(
            flops=0, bytes_accessed=150 * 2**20, transcendentals=0
        ),
        name="moe_scatter",
    )(parts)


def sparse_experts(
    moe_tokens, moe_gain, expert_ids, route_weights, w_gate, w_up, w_down, model_width
):
    lanes = lax.axis_size("tp")
    lane_index = lax.axis_index("tp")
    ep_count = lax.axis_size("ep")
    qrows = moe_tokens.shape[0] // lanes
    top_count = expert_ids.shape[1]
    local_experts = w_gate.shape[0]
    expert_count = local_experts * ep_count
    capacity = max(2, 2 * qrows * top_count // expert_count)
    send_tokens = lax.dynamic_slice_in_dim(moe_tokens, lane_index * qrows, qrows, 0)
    send_ids = lax.dynamic_slice_in_dim(expert_ids, lane_index * qrows, qrows, 0)
    quarters = send_tokens.shape[0] // qrows
    normed = rms_scale(send_tokens.astype(jnp.float32), moe_gain).astype(jnp.bfloat16)
    ids_block = send_ids.reshape(quarters, qrows * top_count)
    ranks = slot_ranks(ids_block, expert_count)
    quarter_base = jnp.arange(quarters, dtype=jnp.int32)[:, None] * (expert_count * capacity)
    slot_index = (quarter_base + ids_block * capacity + ranks).reshape(-1)
    source_row = jnp.arange(quarters * qrows * top_count, dtype=jnp.int32) // top_count
    sources = (
        jnp.full((quarters * expert_count * capacity,), quarters * qrows, jnp.int32)
        .at[slot_index]
        .set(source_row)
    )
    padded = jnp.concatenate([normed, jnp.zeros((1, model_width), jnp.bfloat16)], axis=0)
    outgoing = padded[sources].reshape(quarters, ep_count, local_experts * capacity, model_width)
    arrived = lax.all_to_all(outgoing, "ep", split_axis=1, concat_axis=1, tiled=True)
    piece = lax.all_gather(arrived, "tp", axis=0, tiled=True)
    shaped = piece.reshape(piece.shape[0], ep_count, local_experts, capacity, model_width)
    gate_pre = jnp.einsum("qsecd,edf->qsecf", shaped, w_gate, preferred_element_type=jnp.float32)
    up_pre = jnp.einsum("qsecd,edf->qsecf", shaped, w_up, preferred_element_type=jnp.float32)
    hidden = (jax.nn.silu(gate_pre) * up_pre).astype(jnp.bfloat16)
    lane_rows = ep_count * local_experts * capacity
    projected = jnp.einsum("qsecf,efd->qsecd", hidden, w_down, preferred_element_type=jnp.float32)
    expert_sum = lax.psum_scatter(
        projected.reshape(lax.axis_size("tp") * lane_rows, model_width).astype(jnp.bfloat16),
        "tp",
        scatter_dimension=0,
        tiled=True,
    )
    leaving = expert_sum.reshape(ep_count, local_experts * capacity, model_width)
    returned = lax.all_to_all(leaving, "ep", split_axis=0, concat_axis=0, tiled=True)
    returned = returned.reshape(expert_count * capacity, model_width)
    own_quarter = lane_index * (quarters // lanes)
    own_ids = lax.dynamic_index_in_dim(ids_block, own_quarter, 0, keepdims=False)
    own_ranks = lax.dynamic_index_in_dim(ranks, own_quarter, 0, keepdims=False)
    picked = (
        returned[own_ids * capacity + own_ranks]
        .astype(jnp.float32)
        .reshape(qrows, top_count, model_width)
    )
    own_weights = lax.dynamic_slice_in_dim(route_weights, lane_index * qrows, qrows, 0)
    expert_out = jnp.sum(picked * own_weights[:, :, None], axis=1).astype(jnp.bfloat16)
    return expert_out


def local(
    queries,
    forget_pre,
    value_in,
    out_gate,
    lower_bound,
    out_gain,
    out_weight,
    moe_tokens,
    moe_gain,
    expert_ids,
    route_weights,
    w_gate,
    w_up,
    w_down,
):
    lanes = lax.axis_size("tp")
    ep_count = lax.axis_size("ep")
    model_width = out_weight.shape[1]
    packed = head_states(forget_pre, value_in, lower_bound)
    tokens, top_count = expert_ids.shape
    dense_slots = 2 * (tokens // lanes) * top_count * lanes
    dense = lanes == 4 and ep_count % 2 == 0 and tokens * ep_count <= dense_slots
    if dense:
        experts = w_gate.shape[0] * ep_count
        full = prepare(moe_tokens, moe_gain, expert_ids, route_weights, experts)
        full, packed = lax.optimization_barrier((full, packed))
    gathered = lax.all_gather(packed, "ep")
    if dense:
        parts = moe_gather(full, w_gate, w_up, w_down, ep_count, experts)
        gathered, parts = lax.optimization_barrier((gathered, parts))
    gated = mix_heads(
        gathered, queries, forget_pre, value_in, out_gate, lower_bound, out_gain
    )
    mixer_part = jnp.dot(gated, out_weight, preferred_element_type=jnp.float32).astype(
        jnp.bfloat16
    )
    if dense:
        mixer_part, parts = lax.optimization_barrier((mixer_part, parts))
    mixer_sum = lax.psum_scatter(mixer_part, "tp", scatter_dimension=0, tiled=True)
    if dense:
        expert_out = moe_scatter(parts)
    else:
        expert_out = sparse_experts(
            moe_tokens, moe_gain, expert_ids, route_weights, w_gate, w_up, w_down, model_width
        )
    return (mixer_sum, expert_out)


def solution(mesh):
    in_specs = (
        P("ep", "tp"),
        P("ep", "tp"),
        P("ep", "tp"),
        P("ep", "tp"),
        P("tp"),
        P(),
        P("tp", None),
        P("ep", None),
        P(),
        P("ep", None),
        P("ep", None),
        P("ep", None, "tp"),
        P("ep", None, "tp"),
        P("ep", "tp", None),
    )
    out_specs = (P(("ep", "tp"), None), P(("ep", "tp"), None))
    return jax.shard_map(local, mesh=mesh, in_specs=in_specs, out_specs=out_specs, check_vma=False)
```
